32 devices in a mesh: grp: 2 (over y), kv: 4 (over z), tp: 4 (over x, core).
Axes of the slice: x: 2, y: 2, z: 4, core: 2. Of those that a mesh axis runs over, the one named last changes fastest.
Arguments:
- tokens: bfloat16 [8, 3, 4096], P(('grp', 'kv')), parts along dimension 0, may hold values from -6 to 6
- input_norm_scale: float32 [4096], replicated, may hold values from 0.1 to 1.9
- head_input_matrix: bfloat16 [4096, 8192], P('kv', 'tp'), may hold values from -0.09375 to 0.09375
- output_gate_matrix: bfloat16 [4096, 8192], P('kv', 'tp'), may hold values from -0.09375 to 0.09375
- group_input_matrix: bfloat16 [4096, 512], P('kv', 'tp'), may hold values from -0.09375 to 0.09375
- group_readout_matrix: bfloat16 [4096, 512], P('kv', 'tp'), may hold values from -0.09375 to 0.09375
- step_size_matrix: bfloat16 [4096, 128], P(None, 'tp'), may hold values from -0.09375 to 0.09375
- step_size_bias: float32 [128], P('tp'), may hold values from -4 to -1
- log_decay_rate: float32 [128], P('tp'), may hold values from -4.6 to 2
- direct_path_weight: float32 [128], P('tp'), may hold values from 0.1 to 1.9
- convolution_tap_weight: bfloat16 [4, 8, 1152], P(None, 'tp'), may hold values from -3 to 3
- convolution_history_rows: bfloat16 [8, 6, 8, 1152], P(('grp', 'kv'), None, 'tp'), parts along dimension 0, may hold values from -6 to 6
- per_proposal_states: float32 [8, 3, 128, 64, 64], P(('grp', 'kv'), None, 'tp'), parts along dimension 0, may hold values from -4 to 4
- accepted: int32 [8], P(('grp', 'kv')), parts along dimension 0, may hold values from 1 to 3
- proposal_extra_decay: float32 [8, 3, 128], P(('grp', 'kv'), None, 'tp'), parts along dimension 0, may hold values from -0.69 to 0
- group_norm_scale: float32 [8192], P('tp'), may hold values from 0.1 to 1.9
- output_projection_matrix: bfloat16 [8192, 4096], P('tp', 'kv'), may hold values from -0.0625 to 0.0625
Outputs:
- mixed: bfloat16 [8, 3, 4096], P(('grp', 'tp'), None, 'kv'), parts along dimension 0
- new_states: float32 [8, 3, 128, 64, 64], P(('grp', 'kv'), None, 'tp'), parts along dimension 0
- new_tail: bfloat16 [8, 6, 8, 1152], P(('grp', 'kv'), None, 'tp'), parts along dimension 0
The draws below stay inside these ranges and needn't reach their ends.
There are 2 independent parts, one for each index of `grp`. The reference program is written for one: setup_inputs(seed, part) draws one part's arguments, and reference() takes and returns one part's arrays. A program takes and returns all parts, laid end to end along the dimension named above; an argument that names none is the same for every part. Nothing has to cross between parts.
All inputs are finite; a program needn't handle non-finite values.
Results may differ from the reference program's by a relative error of at most 0.015.
Values may be sent and summed in bfloat16 or wider, within the bound.
A program may use at most 64 MiB of HBM per device.

```python
import jax
import jax.numpy as jnp
from jax import lax

D = 4096
HEADS = 128
HEAD_DIM = 64
GROUPS = 8
STATE = 64
CONV_W = 4
PROP = 3
SEQS = 4
GROUP_CH = 1152
TAIL = 6
N_TP = 4


def draw_proposal_extra_decay(key, part):
    first_key, second_key = jax.random.split(jax.random.fold_in(key, 11))
    struck = jax.random.uniform(first_key, (SEQS, PROP, HEADS), jnp.float32) < 0.15
    depth = jax.random.uniform(second_key, (SEQS, PROP, HEADS), jnp.float32, 0.22, 0.69)
    return jnp.where(struck, -depth, 0.0).astype(jnp.float32)


def touch_ends(result, stream_key, least, largest):
    longest = result.shape.index(max(result.shape))
    spots = []
    for shift in (0, 1):
        where = [jax.random.randint(jax.random.fold_in(stream_key, axis), (), 0, length) for axis, length in enumerate(result.shape)]
        where[longest] = (where[longest] + shift) % result.shape[longest]
        spots.append(tuple(where))
    return result.at[spots[0]].set(least).at[spots[1]].set(largest)


def block_scale(stream_key, extent, pieces, smallest, top_value):
    level, own = 1.0, jax.random.fold_in(stream_key, 6)
    for axis_at, parts in pieces:
        heights = jnp.exp(jax.random.uniform(jax.random.fold_in(own, axis_at), (parts,), jnp.float32, smallest / len(pieces), top_value / len(pieces)))
        level = level * jnp.repeat(heights, extent[axis_at] // parts).reshape([-1 if axis == axis_at else 1 for axis in range(len(extent))])
    return level


def noise(rng, extent, deviation, reach, cuts=(), kind=jnp.bfloat16):
    gain = block_scale(rng, extent, cuts, -0.22, 0.18) if cuts else 1.0
    entries = jax.random.normal(rng, extent, jnp.float32) * deviation * gain
    return jnp.minimum(jnp.maximum(entries, -reach), reach).astype(kind)


def setup_inputs(seed: int = 0, part: int = 0) -> dict:
    key_of = jax.random.split(jax.random.key(seed), 18)
    part_splits = jax.random.split(jax.random.fold_in(key_of[17], part), 18)
    tokens = noise(part_splits[0], (SEQS, PROP, D), 1.0, 6.0, ((0, 4),))
    input_norm_scale = jnp.clip(1.0 + 0.18 * jax.random.normal(key_of[1], (D,), jnp.float32), 0.1, 1.9)
    head_input_matrix = noise(key_of[2], (D, HEADS * HEAD_DIM), D ** -0.5, 0.09375, ((0, 4), (1, 4)))
    output_gate_matrix = noise(key_of[3], (D, HEADS * HEAD_DIM), D ** -0.5, 0.09375, ((0, 4), (1, 4)))
    group_input_matrix = noise(key_of[4], (D, GROUPS * STATE), D ** -0.5, 0.09375, ((0, 4), (1, 4)))
    group_readout_matrix = noise(key_of[5], (D, GROUPS * STATE), D ** -0.5, 0.09375, ((0, 4), (1, 4)))
    step_size_matrix = noise(key_of[6], (D, HEADS), D ** -0.5, 0.09375, ((1, 4),))
    step_size_bias = jnp.clip(-4.0 + 3.0 * jax.random.uniform(key_of[7], (HEADS,), jnp.float32) ** block_scale(key_of[7], (HEADS,), ((0, 4),), -0.2, 0.2), -4.0, -1.0)
    log_decay_rate = jnp.clip(-4.6 + 6.6 * jax.random.uniform(key_of[8], (HEADS,), jnp.float32) ** block_scale(key_of[8], (HEADS,), ((0, 4),), -0.2, 0.2), -4.6, 2.0)
    direct_path_weight = jnp.clip(1.0 + 0.18 * jax.random.normal(key_of[9], (HEADS,), jnp.float32), 0.1, 1.9)
    convolution_tap_weight = noise(key_of[10], (CONV_W, GROUPS, GROUP_CH), 0.5, 3.0, ((1, 4),))
    convolution_history_rows = noise(part_splits[11], (SEQS, TAIL, GROUPS, GROUP_CH), 1.0, 6.0, ((0, 4), (2, 4)))
    per_proposal_states = noise(part_splits[12], (SEQS, PROP, HEADS, HEAD_DIM, STATE), 0.5, 4.0, ((0, 4), (2, 4)), jnp.float32)
    accepted = touch_ends(jax.random.randint(part_splits[13], (SEQS,), 1, PROP + 1), jax.random.fold_in(part_splits[13], 1), 1, PROP).astype(jnp.int32)
    proposal_extra_decay = draw_proposal_extra_decay(jax.random.fold_in(jax.random.fold_in(key_of[17], part), 71), part)
    group_norm_scale = jnp.clip(1.0 + 0.18 * jax.random.normal(key_of[15], (HEADS * HEAD_DIM,), jnp.float32), 0.1, 1.9)
    output_projection_matrix = noise(key_of[16], (HEADS * HEAD_DIM, D), (HEADS * HEAD_DIM) ** -0.5, 0.0625, ((0, 4), (1, 4)))
    return {"tokens": tokens, "input_norm_scale": input_norm_scale, "head_input_matrix": head_input_matrix, "output_gate_matrix": output_gate_matrix, "group_input_matrix": group_input_matrix, "group_readout_matrix": group_readout_matrix, "step_size_matrix": step_size_matrix, "step_size_bias": step_size_bias, "log_decay_rate": log_decay_rate, "direct_path_weight": direct_path_weight, "convolution_tap_weight": convolution_tap_weight, "convolution_history_rows": convolution_history_rows, "per_proposal_states": per_proposal_states, "accepted": accepted, "proposal_extra_decay": proposal_extra_decay, "group_norm_scale": group_norm_scale, "output_projection_matrix": output_projection_matrix}


epsilon = 1e-06

def rms_scale(values):
    return lax.rsqrt(lax.optimization_barrier(jnp.mean(values * values, axis=-1, keepdims=True)) + epsilon)

def causal_states(log_decay_factor, head_step_size, ssm_inputs, inject, start_state):
    cumulative = jnp.cumsum(log_decay_factor, axis=1)
    length = log_decay_factor.shape[1]
    lower = (jnp.arange(length)[:, None] >= jnp.arange(length)[None, :])[None, :, :, None]
    spread = cumulative[:, :, None, :] - cumulative[:, None, :, :]
    factors = jnp.where(lower, jnp.exp(jnp.where(lower, spread, 0.0)), 0.0)
    mixing = factors * head_step_size[:, None, :, :]
    carried = jnp.exp(cumulative)[..., None, None] * start_state[:, None]
    return carried + jnp.einsum('sjih,sihp,sihn->sjhpn', mixing, ssm_inputs, inject)

def combine_head_outputs(incoming_token_rows, gate_portion, unactivated_step, step_size_bias, log_decay_rate, direct_path_weight, convolution_tap_weight, convolution_history_rows, per_proposal_states, accepted, proposal_extra_decay, group_norm_scale):
    sequences, proposals, group_count, group_width = incoming_token_rows.shape
    head_count = step_size_bias.shape[0]
    head_dim = per_proposal_states.shape[3]
    state_size = per_proposal_states.shape[4]
    per_group = head_count // group_count
    group_inner = per_group * head_dim
    tap_count = convolution_tap_weight.shape[0]
    offsets = accepted[:, None] + jnp.arange(tap_count - 1, dtype=jnp.int32)[None, :]
    context = jnp.take_along_axis(convolution_history_rows, offsets[:, :, None, None], axis=1)
    convolution_span = jnp.concatenate([context, incoming_token_rows], axis=1)
    widened = convolution_span.astype(jnp.float32)
    convolved = jnp.zeros((sequences, proposals, group_count, group_width), jnp.float32)
    for conv_tap in range(tap_count):
        convolved = convolved + widened[:, conv_tap:conv_tap + proposals] * convolution_tap_weight[conv_tap].astype(jnp.float32)
    activated = jax.nn.silu(convolved)
    ssm_inputs = activated[..., :group_inner].reshape(sequences, proposals, head_count, head_dim)
    inject = jnp.repeat(activated[..., group_inner:group_inner + state_size], per_group, axis=2)
    readout = jnp.repeat(activated[..., group_inner + state_size:], per_group, axis=2)
    head_step_size = jax.nn.softplus(unactivated_step + step_size_bias)
    log_decay_factor = proposal_extra_decay - jnp.exp(log_decay_rate) * head_step_size
    chosen = (accepted - 1)[:, None, None, None, None]
    start_state = jnp.take_along_axis(per_proposal_states, chosen, axis=1)[:, 0]
    running_state_rows = causal_states(log_decay_factor, head_step_size, ssm_inputs, inject, start_state)
    response = jnp.einsum('sjhn,sjhpn->sjhp', readout, running_state_rows) + direct_path_weight[:, None] * ssm_inputs
    gate_raw = gate_portion.astype(jnp.float32).reshape(sequences, proposals, head_count, head_dim)
    gate_applied_output = (response * jax.nn.silu(gate_raw)).reshape(sequences, proposals, group_count, group_inner)
    scaled = gate_applied_output * rms_scale(gate_applied_output) * group_norm_scale.reshape(group_count, group_inner)
    flat_gated = scaled.astype(jnp.bfloat16).reshape(sequences, proposals, head_count * head_dim)
    return (flat_gated, running_state_rows, convolution_span)

def reference(tokens, input_norm_scale, head_input_matrix, output_gate_matrix, group_input_matrix, group_readout_matrix, step_size_matrix, step_size_bias, log_decay_rate, direct_path_weight, convolution_tap_weight, convolution_history_rows, per_proposal_states, accepted, proposal_extra_decay, group_norm_scale, output_projection_matrix):
    widened = tokens.astype(jnp.float32)
    normed = (widened * rms_scale(widened) * input_norm_scale).astype(jnp.bfloat16)
    flattened = normed.reshape(SEQS * PROP, D)

    def project(weight):
        return jnp.dot(flattened, weight, preferred_element_type=jnp.float32).astype(jnp.bfloat16)
    per_group = HEADS // GROUPS
    part_input = project(head_input_matrix).reshape(SEQS, PROP, GROUPS, per_group * HEAD_DIM)
    part_inject = project(group_input_matrix).reshape(SEQS, PROP, GROUPS, STATE)
    part_readout = project(group_readout_matrix).reshape(SEQS, PROP, GROUPS, STATE)
    gate_portion = project(output_gate_matrix).reshape(SEQS, PROP, HEADS * HEAD_DIM)
    unactivated_step = jnp.dot(flattened, step_size_matrix, preferred_element_type=jnp.float32).reshape(SEQS, PROP, HEADS)
    incoming_token_rows = jnp.concatenate([part_input, part_inject, part_readout], axis=-1)
    gate_applied_output, running_state_rows, convolution_span = combine_head_outputs(incoming_token_rows, gate_portion, unactivated_step, step_size_bias, log_decay_rate, direct_path_weight, convolution_tap_weight, convolution_history_rows, per_proposal_states, accepted, proposal_extra_decay, group_norm_scale)
    block_width = HEADS * HEAD_DIM // N_TP
    gathered = gate_applied_output.reshape(SEQS * PROP, HEADS * HEAD_DIM)
    total = jnp.zeros((SEQS * PROP, D), jnp.float32)
    for shard in range(N_TP):
        partial_sum = jnp.dot(gathered[:, shard * block_width:(shard + 1) * block_width], output_projection_matrix[shard * block_width:(shard + 1) * block_width], preferred_element_type=jnp.float32)
        total = total + lax.optimization_barrier(partial_sum.astype(jnp.bfloat16)).astype(jnp.float32)
    mixed = total.astype(jnp.bfloat16).reshape(SEQS, PROP, D)
    return (mixed, running_state_rows, convolution_span)
```

```python
import functools

import jax
import jax.numpy as jnp
from jax import lax
from jax.experimental import pallas as pl
from jax.experimental.pallas import tpu as pltpu
from jax.sharding import PartitionSpec as P

epsilon = 1e-06


def rms_scale(values):
    return lax.rsqrt(jnp.mean(values * values, axis=-1, keepdims=True) + epsilon)


def causal_states(log_decay_factor, head_step_size, ssm_inputs, inject, start_state):
    cumulative = jnp.cumsum(log_decay_factor, axis=1)
    length = log_decay_factor.shape[1]
    lower = (jnp.arange(length)[:, None] >= jnp.arange(length)[None, :])[None, :, :, None]
    spread = cumulative[:, :, None, :] - cumulative[:, None, :, :]
    factors = jnp.where(lower, jnp.exp(jnp.where(lower, spread, 0.0)), 0.0)
    mixing = factors * head_step_size[:, None, :, :]
    carried = jnp.exp(cumulative)[..., None, None] * start_state[:, None]
    return carried + jnp.einsum("sjih,sihp,sihn->sjhpn", mixing, ssm_inputs, inject)


def combine_head_outputs(
    incoming_token_rows,
    gate_portion,
    unactivated_step,
    step_size_bias,
    log_decay_rate,
    direct_path_weight,
    convolution_tap_weight,
    convolution_history_rows,
    per_proposal_states,
    accepted,
    proposal_extra_decay,
    group_norm_scale,
):
    sequences, proposals, group_count, group_width = incoming_token_rows.shape
    head_count = step_size_bias.shape[0]
    head_dim = per_proposal_states.shape[3]
    state_size = per_proposal_states.shape[4]
    per_group = head_count // group_count
    group_inner = per_group * head_dim
    tap_count = convolution_tap_weight.shape[0]
    offsets = accepted[:, None] + jnp.arange(tap_count - 1, dtype=jnp.int32)[None, :]
    context = jnp.take_along_axis(convolution_history_rows, offsets[:, :, None, None], axis=1)
    convolution_span = jnp.concatenate([context, incoming_token_rows], axis=1)
    widened = convolution_span.astype(jnp.float32)
    convolved = jnp.zeros((sequences, proposals, group_count, group_width), jnp.float32)
    for conv_tap in range(tap_count):
        convolved = convolved + widened[
            :, conv_tap : conv_tap + proposals
        ] * convolution_tap_weight[conv_tap].astype(jnp.float32)
    activated = jax.nn.silu(convolved)
    ssm_inputs = activated[..., :group_inner].reshape(sequences, proposals, head_count, head_dim)
    inject = jnp.repeat(activated[..., group_inner : group_inner + state_size], per_group, axis=2)
    readout = jnp.repeat(activated[..., group_inner + state_size :], per_group, axis=2)
    head_step_size = jax.nn.softplus(unactivated_step + step_size_bias)
    log_decay_factor = proposal_extra_decay - jnp.exp(log_decay_rate) * head_step_size
    chosen = (accepted - 1)[:, None, None, None, None]
    start_state = jnp.take_along_axis(per_proposal_states, chosen, axis=1)[:, 0]
    running_state_rows = causal_states(
        log_decay_factor, head_step_size, ssm_inputs, inject, start_state
    )
    response = (
        jnp.einsum("sjhn,sjhpn->sjhp", readout, running_state_rows)
        + direct_path_weight[:, None] * ssm_inputs
    )
    gate_raw = gate_portion.astype(jnp.float32).reshape(sequences, proposals, head_count, head_dim)
    gate_applied_output = (response * jax.nn.silu(gate_raw)).reshape(
        sequences, proposals, group_count, group_inner
    )
    scaled = (
        gate_applied_output
        * rms_scale(gate_applied_output)
        * group_norm_scale.reshape(group_count, group_inner)
    )
    flat_gated = scaled.astype(jnp.bfloat16).reshape(sequences, proposals, head_count * head_dim)
    return (flat_gated, running_state_rows, convolution_span)


def local(
    tokens,
    input_norm_scale,
    head_input_matrix,
    output_gate_matrix,
    group_input_matrix,
    group_readout_matrix,
    step_size_matrix,
    step_size_bias,
    log_decay_rate,
    direct_path_weight,
    convolution_tap_weight,
    convolution_history_rows,
    per_proposal_states,
    accepted,
    proposal_extra_decay,
    group_norm_scale,
    output_projection_matrix,
):
    local_seqs, proposals, width = tokens.shape
    head_local = step_size_bias.shape[0]
    group_local = convolution_tap_weight.shape[1]
    head_dim = per_proposal_states.shape[3]
    state_size = per_proposal_states.shape[4]
    group_inner = head_local // group_local * head_dim
    widened = tokens.astype(jnp.float32)
    normed = (widened * rms_scale(widened) * input_norm_scale).astype(jnp.bfloat16)
    unactivated_step = jnp.einsum(
        "sjd,dh->sjh", normed, step_size_matrix, preferred_element_type=jnp.float32
    )
    pieces = lax.all_to_all(normed, "kv", split_axis=2, concat_axis=0, tiled=True)
    joined = jnp.concatenate(
        [head_input_matrix, group_input_matrix, group_readout_matrix, output_gate_matrix], axis=1
    )
    summed = lax.psum_scatter(
        jnp.einsum("sjd,dc->sjc", pieces, joined, preferred_element_type=jnp.float32),
        "kv",
        scatter_dimension=0,
        tiled=True,
    )
    projected = summed.astype(jnp.bfloat16)
    input_width = head_local * head_dim
    inject_width = group_local * state_size
    part_input = projected[..., :input_width].reshape(
        local_seqs, proposals, group_local, group_inner
    )
    part_inject = projected[..., input_width : input_width + inject_width].reshape(
        local_seqs, proposals, group_local, state_size
    )
    part_readout = projected[
        ..., input_width + inject_width : input_width + 2 * inject_width
    ].reshape(local_seqs, proposals, group_local, state_size)
    gate_portion = projected[..., input_width + 2 * inject_width :]
    incoming_token_rows = jnp.concatenate([part_input, part_inject, part_readout], axis=-1)
    gate_applied_output, running_state_rows, convolution_span = combine_head_outputs(
        incoming_token_rows,
        gate_portion,
        unactivated_step,
        step_size_bias,
        log_decay_rate,
        direct_path_weight,
        convolution_tap_weight,
        convolution_history_rows,
        per_proposal_states,
        accepted,
        proposal_extra_decay,
        group_norm_scale,
    )
    terms = jnp.einsum(
        "sjc,cd->sjd",
        lax.all_gather(gate_applied_output, "kv", axis=0, tiled=True),
        output_projection_matrix,
        preferred_element_type=jnp.float32,
    )
    mixed = lax.psum_scatter(terms.astype(jnp.bfloat16), "tp", scatter_dimension=0, tiled=True)
    return (mixed, running_state_rows, convolution_span)


MESH_ID = pl.DeviceIdType.MESH


def lane_chunks(width, piece):
    return [(lo, min(piece, width - lo)) for lo in range(0, width, piece)]


def split_rows(value):
    high = value.astype(jnp.bfloat16).astype(jnp.float32)
    rest = value - high
    middle = rest.astype(jnp.bfloat16).astype(jnp.float32)
    return high, middle, rest - middle


def mixer_kernel(
    sizes,
    accepted,
    tokens,
    input_scale,
    head_hbm,
    gate_hbm,
    inject_hbm,
    readout_hbm,
    step_hbm,
    step_bias,
    decay_rate,
    direct_weight,
    taps,
    history,
    states_hbm,
    extra_decay,
    norm_scale,
    out_hbm,
    mixed_out,
    states_out,
    tail_out,
    head_w,
    gate_w,
    inject_w,
    readout_w,
    step_w,
    states,
    out_w,
    normed_buf,
    normed_in,
    own_sum,
    sum_buf,
    sum_in,
    gated_buf,
    gated_in,
    out_buf,
    out_in,
    span,
    outer_buf,
    decay_buf,
    load_sem,
    a_send,
    a_recv,
    b_send,
    b_recv,
    c_send,
    c_recv,
    d_send,
    d_recv,
):
    kv, tp, rows, props = sizes
    width = tokens.shape[-1]
    part = width // kv
    heads = step_bias.shape[-1]
    groups, channels = taps.shape[1:]
    head_dim, state = states.shape[2:]
    per_group = heads // groups
    inner = per_group * head_dim
    inputs = heads * head_dim
    bc = groups * state
    taps_n = taps.shape[0]
    f32 = jnp.float32
    bf16 = jnp.bfloat16
    me = lax.axis_index("kv")
    me_tp = lax.axis_index("tp")

    def kv_peer(d):
        return lax.rem(me + d, kv)

    def kv_source(d):
        return lax.rem(me + kv - d, kv)

    loads = []

    def load(src, dst):
        copy = pltpu.make_async_copy(src, dst, load_sem.at[len(loads)])
        copy.start()
        loads.append(copy)
        return copy

    step_load = load(step_hbm, step_w)
    big = lane_chunks(inputs, inputs // 2)
    head_loads = [load(head_hbm.at[:, lo : lo + n], head_w.at[:, lo : lo + n]) for lo, n in big]
    group_loads = [load(inject_hbm, inject_w), load(readout_hbm, readout_w)]
    gate_loads = [load(gate_hbm.at[:, lo : lo + n], gate_w.at[:, lo : lo + n]) for lo, n in big]
    states_load = load(states_hbm.at[0], states)
    out_load = load(out_hbm, out_w)

    barrier = pltpu.get_barrier_semaphore()
    for d in range(1, kv):
        pl.semaphore_signal(barrier, 1, device_id={"kv": kv_peer(d)}, device_id_type=MESH_ID)
    for d in range(1, tp):
        pl.semaphore_signal(
            barrier, 1, device_id={"tp": lax.rem(me_tp + d, tp)}, device_id_type=MESH_ID
        )

    wide = tokens[0].astype(f32)
    normed = wide * rms_scale(wide) * input_scale[...]
    normed = jnp.concatenate([normed, jnp.zeros((rows - props, width), f32)], axis=0)
    for k in range(kv):
        normed_buf[k] = normed[:, k * part : (k + 1) * part].astype(bf16)
    pl.semaphore_wait(barrier, kv + tp - 2)

    copies = []

    def send(src, dst, send_sem, recv_sem, device):
        copy = pltpu.make_async_remote_copy(
            src_ref=src,
            dst_ref=dst,
            send_sem=send_sem,
            recv_sem=recv_sem,
            device_id=device,
            device_id_type=MESH_ID,
        )
        copy.start()
        copies.append(copy)
        return copy

    first = [
        send(normed_buf.at[kv_peer(d)], normed_in.at[d], a_send.at[d], a_recv.at[d], {"kv": kv_peer(d)})
        for d in range(1, kv)
    ]

    step_load.wait()
    step_raw = lax.dot_general(
        normed.astype(bf16), step_w[...], (((1,), (1,)), ((), ())), preferred_element_type=f32
    )[:props]
    biased = step_raw + step_bias[...]
    step_size = jnp.maximum(biased, 0.0) + jnp.log1p(jnp.exp(-jnp.abs(biased)))
    rate = jnp.exp(decay_rate[...])
    log_rows = [extra_decay[j] - rate * step_size[j : j + 1] for j in range(props)]
    cumulative = [log_rows[0]]
    for j in range(1, props):
        cumulative.append(cumulative[-1] + log_rows[j])
    pairs = [(j, i) for j in range(props) for i in range(j + 1)]
    stacked = [jnp.exp(row) for row in cumulative]
    stacked += [jnp.exp(cumulative[j] - cumulative[i]) * step_size[i : i + 1] for j, i in pairs]
    stacked.append(direct_weight[...])
    count = len(stacked)
    table = jnp.concatenate(stacked, axis=0)
    padded = -(-3 * count // 16) * 16
    pieces = list(split_rows(table)) + [jnp.zeros((padded - 3 * count, heads), f32)]
    spread = (
        lax.broadcasted_iota(jnp.int32, (heads, inputs), 1) // head_dim
        == lax.broadcasted_iota(jnp.int32, (heads, inputs), 0)
    )
    wide_table = jnp.dot(
        jnp.concatenate(pieces, axis=0).astype(bf16),
        jnp.where(spread, 1.0, 0.0).astype(bf16),
        preferred_element_type=f32,
    )
    expanded = wide_table[:count] + wide_table[count : 2 * count] + wide_table[2 * count : 3 * count]

    dec = jnp.concatenate([jnp.exp(row) for row in log_rows], axis=0)
    dec = jnp.concatenate([dec, jnp.zeros((8 - props, heads), f32)], axis=0)
    dec = jnp.concatenate([dec, jnp.zeros((8, 128 - heads), f32)], axis=1)
    dec_t = jnp.transpose(dec)
    for j in range(props):
        decay_buf[j] = jnp.broadcast_to(dec_t[:heads, j : j + 1], (heads, state))

    start = jnp.maximum(accepted[0], 1)
    for r in range(taps_n - 1):
        row = history[0, start + r]
        tail_out[0, r] = row
        row = row.astype(f32)
        for g in range(groups):
            span[g, r : r + 1] = row[g : g + 1]

    blocks = [normed_buf[me].astype(f32)]
    for d in range(1, kv):
        first[d - 1].wait_recv()
        blocks.append(normed_in[d].astype(f32))
    gathered = jnp.concatenate(blocks, axis=0).astype(bf16)

    stages = []
    for at, (lo, n) in enumerate(big):
        stages.append((lo, [(head_w, lo, n)], [head_loads[at]]))
    stages.append((inputs, [(inject_w, 0, bc), (readout_w, 0, bc)], group_loads))
    for at, (lo, n) in enumerate(big):
        stages.append((inputs + 2 * bc + lo, [(gate_w, lo, n)], [gate_loads[at]]))
    second = [[] for _ in stages]
    ranges = []

    def send_sums(stage):
        lo, n = ranges[stage]
        for d in range(1, kv):
            second[stage].append(
                send(
                    sum_buf.at[d, :, lo : lo + n],
                    sum_in.at[d, :, lo : lo + n],
                    b_send.at[stage, d],
                    b_recv.at[stage, d],
                    {"kv": kv_source(d)},
                )
            )

    for stage, (base, operands, ready) in enumerate(stages):
        for copy in ready:
            copy.wait()
        at = base
        for ref, lo, n in operands:
            for sub, size in lane_chunks(n, 512):
                part_sum = jnp.dot(
                    gathered, ref[:, lo + sub : lo + sub + size], preferred_element_type=f32
                )
                own_sum[:, at : at + size] = part_sum[:rows]
                for d in range(1, kv):
                    sum_buf[d, :, at : at + size] = part_sum[d * rows : (d + 1) * rows].astype(bf16)
                at += size
        ranges.append((base, at - base))
        if stage:
            send_sums(stage - 1)
    states_load.wait()
    send_sums(len(stages) - 1)

    def summed(stage):
        lo, n = ranges[stage]
        total = own_sum[:, lo : lo + n]
        for d in range(1, kv):
            second[stage][d - 1].wait_recv()
            total = total + sum_in[d, :, lo : lo + n].astype(f32)
        return total.astype(bf16).astype(f32)[:props]

    part_x = jnp.concatenate([summed(s) for s in range(len(big))], axis=1)
    part_bc = summed(len(big))
    fresh = []
    for g in range(groups):
        fresh.append(
            jnp.concatenate(
                [
                    part_x[:, g * inner : (g + 1) * inner],
                    part_bc[:, g * state : (g + 1) * state],
                    part_bc[:, bc + g * state : bc + (g + 1) * state],
                ],
                axis=1,
            )
        )
        span[g, taps_n - 1 : taps_n - 1 + props] = fresh[g]
    for j in range(props):
        tail_out[0, taps_n - 1 + j] = jnp.concatenate(
            [fresh[g][j : j + 1] for g in range(groups)], axis=0
        ).astype(bf16)

    lhs_rows = [None] * groups
    rhs = [None] * groups
    responses = []
    for g in range(groups):
        conv = jnp.zeros((props, channels), f32)
        for k in range(taps_n):
            conv = conv + span[g, k : k + props] * taps[k].astype(f32)[g : g + 1]
        act = conv * jax.nn.sigmoid(conv)
        x = act[:, :inner]
        b = act[:, inner : inner + state]
        c = act[:, inner + state :]
        cols = slice(g * inner, (g + 1) * inner)
        previous = states[start - 1, g * per_group : (g + 1) * per_group].reshape(inner, state)
        carried = lax.dot_general(
            jnp.concatenate([c, jnp.zeros((16 - props, state), f32)], axis=0).astype(bf16),
            previous.astype(bf16),
            (((1,), (1,)), ((), ())),
            preferred_element_type=f32,
        )
        out_rows = []
        for j in range(props):
            total = expanded[j : j + 1, cols] * carried[j : j + 1]
            total = total + expanded[count - 1 : count, cols] * x[j : j + 1]
            for i in range(j + 1):
                weight = jnp.sum(b[i : i + 1] * c[j : j + 1], axis=-1, keepdims=True)
                at = props + pairs.index((j, i))
                total = total + expanded[at : at + 1, cols] * weight * x[i : i + 1]
            out_rows.append(total)
        responses.append(jnp.concatenate(out_rows, axis=0))
        left, right = [], []
        for j in range(props):
            at = props + pairs.index((j, j))
            scaled = expanded[at : at + 1, cols] * x[j : j + 1]
            xh, xm, _ = split_rows(scaled)
            bh, bm, _ = split_rows(b[j : j + 1])
            left += [xh, xh, xm]
            before = jnp.zeros((1, 128 * j), f32)
            after = jnp.zeros((1, 128 * (props - j) - state), f32)
            for row in (bh, bm, bh):
                right.append(jnp.concatenate(([before] if j else []) + [row, after], axis=1))
        extra = -len(left) % 16
        lhs_rows[g] = jnp.concatenate(left + [jnp.zeros((extra, inner), f32)], axis=0)
        rhs[g] = jnp.concatenate(right + [jnp.zeros((extra, 128 * props), f32)], axis=0)

    gate = jnp.concatenate([summed(len(big) + 1 + s) for s in range(len(big))], axis=1)
    for g in range(groups):
        cols = slice(g * inner, (g + 1) * inner)
        raw = gate[:, cols]
        value = responses[g] * (raw * jax.nn.sigmoid(raw))
        value = value * rms_scale(value) * norm_scale[:, cols]
        value = jnp.concatenate([value, jnp.zeros((rows - props, inner), f32)], axis=0)
        gated_buf[:, cols] = value.astype(bf16)

    for g in range(groups):
        outer_buf[g * inner : (g + 1) * inner] = jnp.dot(
            jnp.transpose(lhs_rows[g]).astype(bf16), rhs[g].astype(bf16), preferred_element_type=f32
        )
        if g == 0:
            third = [
                send(gated_buf, gated_in.at[d], c_send.at[d], c_recv.at[d], {"kv": kv_peer(d)})
                for d in range(1, kv)
            ]

    def head_step(h, _):
        value = states[start - 1, h]
        for j in range(props):
            outer = outer_buf[pl.ds(pl.multiple_of(h * head_dim, head_dim), head_dim), 128 * j : 128 * j + state]
            value = value * decay_buf[j, pl.ds(h, 1)] + outer
            states_out[0, j, h] = value
        return 0

    lax.fori_loop(0, heads, head_step, 0, unroll=4)

    out_load.wait()
    blocks = [gated_buf[...].astype(f32)]
    for d in range(1, kv):
        third[d - 1].wait_recv()
        blocks.append(gated_in[d].astype(f32))
    everyone = jnp.concatenate(blocks, axis=0).astype(bf16)
    fourth = []
    for sub, size in lane_chunks(out_w.shape[1], 512):
        product = jnp.dot(everyone, out_w[:, sub : sub + size], preferred_element_type=f32)
        for d in range(kv):
            out_buf[d, :, sub : sub + size] = product[d * rows : (d + 1) * rows].astype(bf16)
    for d in range(1, tp):
        target = lax.rem(me_tp + d, tp)
        fourth.append(
            send(
                out_buf.at[lax.rem(me + kv - target, kv)],
                out_in.at[d],
                d_send.at[d],
                d_recv.at[d],
                {"tp": target},
            )
        )
    total = out_buf[lax.rem(me + kv - me_tp, kv)].astype(f32)
    for d in range(1, tp):
        fourth[d - 1].wait_recv()
        total = total + out_in[d].astype(f32)
    mixed_out[0] = total[:props].astype(bf16)
    for copy in copies:
        copy.wait_send()


def fused(kv, tp, args):
    (
        tokens,
        input_norm_scale,
        head_input_matrix,
        output_gate_matrix,
        group_input_matrix,
        group_readout_matrix,
        step_size_matrix,
        step_size_bias,
        log_decay_rate,
        direct_path_weight,
        convolution_tap_weight,
        convolution_history_rows,
        per_proposal_states,
        accepted,
        proposal_extra_decay,
        group_norm_scale,
        output_projection_matrix,
    ) = args
    _, props, width = tokens.shape
    rows = -(-props // 4) * 4
    heads = step_size_bias.shape[0]
    groups, channels = convolution_tap_weight.shape[1:]
    state = per_proposal_states.shape[4]
    inputs = head_input_matrix.shape[1]
    total = 2 * inputs + 2 * group_input_matrix.shape[1]
    columns = output_projection_matrix.shape[1]
    bf16, f32 = jnp.bfloat16, jnp.float32
    stages = 5
    vmem = pl.BlockSpec(memory_space=pltpu.VMEM)
    hbm = pl.BlockSpec(memory_space=pl.ANY)
    smem = pl.BlockSpec(memory_space=pltpu.SMEM)
    dma = pltpu.SemaphoreType.DMA
    return pl.pallas_call(
        functools.partial(mixer_kernel, (kv, tp, rows, props)),
        name="mixer",
        out_shape=(
            jax.ShapeDtypeStruct((1, props, columns), bf16),
            jax.ShapeDtypeStruct(per_proposal_states.shape, f32),
            jax.ShapeDtypeStruct(convolution_history_rows.shape, bf16),
        ),
        in_specs=[
            smem, vmem, vmem, hbm, hbm, hbm, hbm, hbm,
            vmem, vmem, vmem, vmem, vmem, hbm, vmem, vmem, hbm,
        ],
        out_specs=(vmem, vmem, vmem),
        scratch_shapes=[
            pltpu.VMEM(head_input_matrix.shape, bf16),
            pltpu.VMEM(output_gate_matrix.shape, bf16),
            pltpu.VMEM(group_input_matrix.shape, bf16),
            pltpu.VMEM(group_readout_matrix.shape, bf16),
            pltpu.VMEM(step_size_matrix.shape[::-1], bf16),
            pltpu.VMEM(per_proposal_states.shape[1:], f32),
            pltpu.VMEM(output_projection_matrix.shape, bf16),
            pltpu.VMEM((kv, rows, width // kv), bf16),
            pltpu.VMEM((kv, rows, width // kv), bf16),
            pltpu.VMEM((rows, total), f32),
            pltpu.VMEM((kv, rows, total), bf16),
            pltpu.VMEM((kv, rows, total), bf16),
            pltpu.VMEM((rows, inputs), bf16),
            pltpu.VMEM((kv, rows, inputs), bf16),
            pltpu.VMEM((kv, rows, columns), bf16),
            pltpu.VMEM((tp, rows, columns), bf16),
            pltpu.VMEM((groups, 8, channels), f32),
            pltpu.VMEM((inputs, 128 * props), f32),
            pltpu.VMEM((props, heads, state), f32),
            dma((9,)),
            dma((kv,)),
            dma((kv,)),
            dma((stages, kv)),
            dma((stages, kv)),
            dma((kv,)),
            dma((kv,)),
            dma((tp,)),
            dma((tp,)),
        ],
        compiler_params=pltpu.CompilerParams(
            collective_id=0, has_side_effects=True, vmem_limit_bytes=60 * 1024 * 1024
        ),
    )(
        accepted,
        tokens,
        input_norm_scale[None],
        head_input_matrix,
        output_gate_matrix,
        group_input_matrix,
        group_readout_matrix,
        step_size_matrix.T,
        step_size_bias[None],
        log_decay_rate[None],
        direct_path_weight[None],
        convolution_tap_weight,
        convolution_history_rows,
        per_proposal_states,
        jnp.transpose(proposal_extra_decay, (1, 0, 2)),
        group_norm_scale[None],
        output_projection_matrix,
    )


def fits(kv, tp, args):
    tokens, taps, states = args[0], args[10], args[12]
    heads = args[7].shape[0]
    slices = (tokens.shape[2] // kv, args[4].shape[1], args[16].shape[1])
    return (
        kv == tp
        and tokens.shape[0] == 1
        and tokens.shape[1] + taps.shape[0] - 1 <= 8
        and heads <= 128
        and states.shape[4] <= 128
        and heads // taps.shape[1] * states.shape[3] % 128 == 0
        and all(n % 128 == 0 for n in slices)
        and args[2].shape[1] % 256 == 0
    )


def solution(mesh):
    kv, tp = mesh.shape["kv"], mesh.shape["tp"]

    def body(*args):
        if fits(kv, tp, args):
            return tuple(fused(kv, tp, args))
        return local(*args)

    return jax.shard_map(
        body,
        mesh=mesh,
        in_specs=(
            P(("grp", "kv"), None, None),
            P(),
            P("kv", "tp"),
            P("kv", "tp"),
            P("kv", "tp"),
            P("kv", "tp"),
            P(None, "tp"),
            P("tp"),
            P("tp"),
            P("tp"),
            P(None, "tp", None),
            P(("grp", "kv"), None, "tp", None),
            P(("grp", "kv"), None, "tp", None, None),
            P(("grp", "kv")),
            P(("grp", "kv"), None, "tp"),
            P("tp"),
            P("tp", "kv"),
        ),
        out_specs=(
            P(("grp", "tp"), None, "kv"),
            P(("grp", "kv"), None, "tp", None, None),
            P(("grp", "kv"), None, "tp", None),
        ),
        check_vma=False,
    )
```

```python
import functools

import jax
import jax.numpy as jnp
from jax import lax
from jax.experimental import pallas as pl
from jax.experimental.pallas import tpu as pltpu
from jax.sharding import PartitionSpec as P

epsilon = 1e-06


def rms_scale(values):
    return lax.rsqrt(jnp.mean(values * values, axis=-1, keepdims=True) + epsilon)


def causal_states(log_decay_factor, head_step_size, ssm_inputs, inject, start_state):
    cumulative = jnp.cumsum(log_decay_factor, axis=1)
    length = log_decay_factor.shape[1]
    lower = (jnp.arange(length)[:, None] >= jnp.arange(length)[None, :])[None, :, :, None]
    spread = cumulative[:, :, None, :] - cumulative[:, None, :, :]
    factors = jnp.where(lower, jnp.exp(jnp.where(lower, spread, 0.0)), 0.0)
    mixing = factors * head_step_size[:, None, :, :]
    carried = jnp.exp(cumulative)[..., None, None] * start_state[:, None]
    return carried + jnp.einsum("sjih,sihp,sihn->sjhpn", mixing, ssm_inputs, inject)


def combine_head_outputs(
    incoming_token_rows,
    gate_portion,
    unactivated_step,
    step_size_bias,
    log_decay_rate,
    direct_path_weight,
    convolution_tap_weight,
    convolution_history_rows,
    per_proposal_states,
    accepted,
    proposal_extra_decay,
    group_norm_scale,
):
    sequences, proposals, group_count, group_width = incoming_token_rows.shape
    head_count = step_size_bias.shape[0]
    head_dim = per_proposal_states.shape[3]
    state_size = per_proposal_states.shape[4]
    per_group = head_count // group_count
    group_inner = per_group * head_dim
    tap_count = convolution_tap_weight.shape[0]
    offsets = accepted[:, None] + jnp.arange(tap_count - 1, dtype=jnp.int32)[None, :]
    context = jnp.take_along_axis(convolution_history_rows, offsets[:, :, None, None], axis=1)
    convolution_span = jnp.concatenate([context, incoming_token_rows], axis=1)
    widened = convolution_span.astype(jnp.float32)
    convolved = jnp.zeros((sequences, proposals, group_count, group_width), jnp.float32)
    for conv_tap in range(tap_count):
        convolved = convolved + widened[
            :, conv_tap : conv_tap + proposals
        ] * convolution_tap_weight[conv_tap].astype(jnp.float32)
    activated = jax.nn.silu(convolved)
    ssm_inputs = activated[..., :group_inner].reshape(sequences, proposals, head_count, head_dim)
    inject = jnp.repeat(activated[..., group_inner : group_inner + state_size], per_group, axis=2)
    readout = jnp.repeat(activated[..., group_inner + state_size :], per_group, axis=2)
    head_step_size = jax.nn.softplus(unactivated_step + step_size_bias)
    log_decay_factor = proposal_extra_decay - jnp.exp(log_decay_rate) * head_step_size
    chosen = (accepted - 1)[:, None, None, None, None]
    start_state = jnp.take_along_axis(per_proposal_states, chosen, axis=1)[:, 0]
    running_state_rows = causal_states(
        log_decay_factor, head_step_size, ssm_inputs, inject, start_state
    )
    response = (
        jnp.einsum("sjhn,sjhpn->sjhp", readout, running_state_rows)
        + direct_path_weight[:, None] * ssm_inputs
    )
    gate_raw = gate_portion.astype(jnp.float32).reshape(sequences, proposals, head_count, head_dim)
    gate_applied_output = (response * jax.nn.silu(gate_raw)).reshape(
        sequences, proposals, group_count, group_inner
    )
    scaled = (
        gate_applied_output
        * rms_scale(gate_applied_output)
        * group_norm_scale.reshape(group_count, group_inner)
    )
    flat_gated = scaled.astype(jnp.bfloat16).reshape(sequences, proposals, head_count * head_dim)
    return (flat_gated, running_state_rows, convolution_span)


def local(
    tokens,
    input_norm_scale,
    head_input_matrix,
    output_gate_matrix,
    group_input_matrix,
    group_readout_matrix,
    step_size_matrix,
    step_size_bias,
    log_decay_rate,
    direct_path_weight,
    convolution_tap_weight,
    convolution_history_rows,
    per_proposal_states,
    accepted,
    proposal_extra_decay,
    group_norm_scale,
    output_projection_matrix,
):
    local_seqs, proposals, width = tokens.shape
    head_local = step_size_bias.shape[0]
    group_local = convolution_tap_weight.shape[1]
    head_dim = per_proposal_states.shape[3]
    state_size = per_proposal_states.shape[4]
    group_inner = head_local // group_local * head_dim
    widened = tokens.astype(jnp.float32)
    normed = (widened * rms_scale(widened) * input_norm_scale).astype(jnp.bfloat16)
    unactivated_step = jnp.einsum(
        "sjd,dh->sjh", normed, step_size_matrix, preferred_element_type=jnp.float32
    )
    pieces = lax.all_to_all(normed, "kv", split_axis=2, concat_axis=0, tiled=True)
    joined = jnp.concatenate(
        [head_input_matrix, group_input_matrix, group_readout_matrix, output_gate_matrix], axis=1
    )
    summed = lax.psum_scatter(
        jnp.einsum("sjd,dc->sjc", pieces, joined, preferred_element_type=jnp.float32),
        "kv",
        scatter_dimension=0,
        tiled=True,
    )
    projected = summed.astype(jnp.bfloat16)
    input_width = head_local * head_dim
    inject_width = group_local * state_size
    part_input = projected[..., :input_width].reshape(
        local_seqs, proposals, group_local, group_inner
    )
    part_inject = projected[..., input_width : input_width + inject_width].reshape(
        local_seqs, proposals, group_local, state_size
    )
    part_readout = projected[
        ..., input_width + inject_width : input_width + 2 * inject_width
    ].reshape(local_seqs, proposals, group_local, state_size)
    gate_portion = projected[..., input_width + 2 * inject_width :]
    incoming_token_rows = jnp.concatenate([part_input, part_inject, part_readout], axis=-1)
    gate_applied_output, running_state_rows, convolution_span = combine_head_outputs(
        incoming_token_rows,
        gate_portion,
        unactivated_step,
        step_size_bias,
        log_decay_rate,
        direct_path_weight,
        convolution_tap_weight,
        convolution_history_rows,
        per_proposal_states,
        accepted,
        proposal_extra_decay,
        group_norm_scale,
    )
    terms = jnp.einsum(
        "sjc,cd->sjd",
        lax.all_gather(gate_applied_output, "kv", axis=0, tiled=True),
        output_projection_matrix,
        preferred_element_type=jnp.float32,
    )
    mixed = lax.psum_scatter(terms.astype(jnp.bfloat16), "tp", scatter_dimension=0, tiled=True)
    return (mixed, running_state_rows, convolution_span)


MESH_ID = pl.DeviceIdType.MESH


def lane_chunks(width, piece):
    return [(lo, min(piece, width - lo)) for lo in range(0, width, piece)]


def split_rows(value):
    high = value.astype(jnp.bfloat16).astype(jnp.float32)
    rest = value - high
    middle = rest.astype(jnp.bfloat16).astype(jnp.float32)
    return high, middle, rest - middle


def mixer_kernel(
    sizes,
    accepted,
    tokens_hbm,
    input_scale_hbm,
    head_hbm,
    gate_hbm,
    inject_hbm,
    readout_hbm,
    step_hbm,
    step_bias_hbm,
    decay_rate_hbm,
    direct_weight_hbm,
    taps_hbm,
    history_hbm,
    states_hbm,
    extra_decay_hbm,
    norm_scale_hbm,
    out_hbm,
    mixed_out,
    states_out,
    tail_out,
    tokens,
    input_scale,
    step_bias,
    decay_rate,
    direct_weight,
    taps,
    history,
    extra_decay,
    norm_scale,
    head_w,
    gate_w,
    inject_w,
    readout_w,
    step_w,
    states,
    out_w,
    normed_buf,
    normed_in,
    own_sum,
    sum_buf,
    sum_in,
    gated_buf,
    gated_in,
    out_buf,
    out_in,
    span,
    outer_buf,
    decay_buf,
    load_sem,
    a_send,
    a_recv,
    b_send,
    b_recv,
    c_send,
    c_recv,
    d_send,
    d_recv,
):
    kv, tp, rows, props = sizes
    width = tokens.shape[-1]
    part = width // kv
    heads = step_bias.shape[-1]
    groups, channels = taps.shape[1:]
    head_dim, state = states.shape[2:]
    per_group = heads // groups
    inner = per_group * head_dim
    inputs = heads * head_dim
    bc = groups * state
    taps_n = taps.shape[0]
    f32 = jnp.float32
    bf16 = jnp.bfloat16
    me = lax.axis_index("kv")
    me_tp = lax.axis_index("tp")

    def kv_peer(d):
        return lax.rem(me + d, kv)

    def kv_source(d):
        return lax.rem(me + kv - d, kv)

    barrier = pltpu.get_barrier_semaphore()
    for d in range(1, kv):
        pl.semaphore_signal(barrier, 1, device_id={"kv": kv_peer(d)}, device_id_type=MESH_ID)
    for d in range(1, tp):
        pl.semaphore_signal(
            barrier, 1, device_id={"tp": lax.rem(me_tp + d, tp)}, device_id_type=MESH_ID
        )

    loads = []

    def load(src, dst):
        copy = pltpu.make_async_copy(src, dst, load_sem.at[len(loads)])
        copy.start()
        loads.append(copy)
        return copy

    token_loads = [load(tokens_hbm, tokens), load(input_scale_hbm, input_scale)]
    step_loads = [
        load(step_hbm, step_w),
        load(step_bias_hbm, step_bias),
        load(decay_rate_hbm, decay_rate),
        load(direct_weight_hbm, direct_weight),
        load(extra_decay_hbm, extra_decay),
    ]
    row_loads = [
        load(history_hbm, history),
        load(taps_hbm, taps),
        load(norm_scale_hbm, norm_scale),
    ]
    big = lane_chunks(inputs, inputs // 2)
    head_loads = [load(head_hbm.at[:, lo : lo + n], head_w.at[:, lo : lo + n]) for lo, n in big]
    group_loads = [load(inject_hbm, inject_w), load(readout_hbm, readout_w)]
    gate_loads = [load(gate_hbm.at[:, lo : lo + n], gate_w.at[:, lo : lo + n]) for lo, n in big]
    states_load = load(states_hbm.at[0], states)
    out_load = load(out_hbm, out_w)

    for copy in token_loads:
        copy.wait()
    wide = tokens[0].astype(f32)
    normed = wide * rms_scale(wide) * input_scale[...]
    normed = jnp.concatenate([normed, jnp.zeros((rows - props, width), f32)], axis=0)
    for k in range(kv):
        normed_buf[k] = normed[:, k * part : (k + 1) * part].astype(bf16)
    pl.semaphore_wait(barrier, kv + tp - 2)

    copies = []

    def send(src, dst, send_sem, recv_sem, device):
        copy = pltpu.make_async_remote_copy(
            src_ref=src,
            dst_ref=dst,
            send_sem=send_sem,
            recv_sem=recv_sem,
            device_id=device,
            device_id_type=MESH_ID,
        )
        copy.start()
        copies.append(copy)
        return copy

    first = [
        send(normed_buf.at[kv_peer(d)], normed_in.at[d], a_send.at[d], a_recv.at[d], {"kv": kv_peer(d)})
        for d in range(1, kv)
    ]

    for copy in step_loads:
        copy.wait()
    step_raw = lax.dot_general(
        normed.astype(bf16), step_w[...], (((1,), (1,)), ((), ())), preferred_element_type=f32
    )[:props]
    biased = step_raw + step_bias[...]
    step_size = jnp.maximum(biased, 0.0) + jnp.log1p(jnp.exp(-jnp.abs(biased)))
    rate = jnp.exp(decay_rate[...])
    log_rows = [extra_decay[j] - rate * step_size[j : j + 1] for j in range(props)]
    cumulative = [log_rows[0]]
    for j in range(1, props):
        cumulative.append(cumulative[-1] + log_rows[j])
    pairs = [(j, i) for j in range(props) for i in range(j + 1)]
    stacked = [jnp.exp(row) for row in cumulative]
    stacked += [jnp.exp(cumulative[j] - cumulative[i]) * step_size[i : i + 1] for j, i in pairs]
    stacked.append(direct_weight[...])
    count = len(stacked)
    table = jnp.concatenate(stacked, axis=0)
    padded = -(-3 * count // 16) * 16
    pieces = list(split_rows(table)) + [jnp.zeros((padded - 3 * count, heads), f32)]
    spread = (
        lax.broadcasted_iota(jnp.int32, (heads, inputs), 1) // head_dim
        == lax.broadcasted_iota(jnp.int32, (heads, inputs), 0)
    )
    wide_table = jnp.dot(
        jnp.concatenate(pieces, axis=0).astype(bf16),
        jnp.where(spread, 1.0, 0.0).astype(bf16),
        preferred_element_type=f32,
    )
    expanded = wide_table[:count] + wide_table[count : 2 * count] + wide_table[2 * count : 3 * count]

    dec = jnp.concatenate([jnp.exp(row) for row in log_rows], axis=0)
    dec = jnp.concatenate([dec, jnp.zeros((8 - props, heads), f32)], axis=0)
    dec = jnp.concatenate([dec, jnp.zeros((8, 128 - heads), f32)], axis=1)
    dec_t = jnp.transpose(dec)
    for j in range(props):
        decay_buf[j] = jnp.broadcast_to(dec_t[:heads, j : j + 1], (heads, state))

    for copy in row_loads:
        copy.wait()
    start = jnp.maximum(accepted[0], 1)
    for r in range(taps_n - 1):
        row = history[0, start + r]
        tail_out[0, r] = row
        row = row.astype(f32)
        for g in range(groups):
            span[g, r : r + 1] = row[g : g + 1]

    blocks = [normed_buf[me].astype(f32)]
    for d in range(1, kv):
        first[d - 1].wait_recv()
        blocks.append(normed_in[d].astype(f32))
    gathered = jnp.concatenate(blocks, axis=0).astype(bf16)

    stages = []
    for at, (lo, n) in enumerate(big):
        stages.append((lo, [(head_w, lo, n)], [head_loads[at]]))
    stages.append((inputs, [(inject_w, 0, bc), (readout_w, 0, bc)], group_loads))
    for at, (lo, n) in enumerate(big):
        stages.append((inputs + 2 * bc + lo, [(gate_w, lo, n)], [gate_loads[at]]))
    second = [[] for _ in stages]
    ranges = []

    def send_sums(stage):
        lo, n = ranges[stage]
        for d in range(1, kv):
            second[stage].append(
                send(
                    sum_buf.at[d, :, lo : lo + n],
                    sum_in.at[d, :, lo : lo + n],
                    b_send.at[stage, d],
                    b_recv.at[stage, d],
                    {"kv": kv_source(d)},
                )
            )

    for stage, (base, operands, ready) in enumerate(stages):
        for copy in ready:
            copy.wait()
        at = base
        for ref, lo, n in operands:
            for sub, size in lane_chunks(n, 512):
                part_sum = jnp.dot(
                    gathered, ref[:, lo + sub : lo + sub + size], preferred_element_type=f32
                )
                own_sum[:, at : at + size] = part_sum[:rows]
                for d in range(1, kv):
                    sum_buf[d, :, at : at + size] = part_sum[d * rows : (d + 1) * rows].astype(bf16)
                at += size
        ranges.append((base, at - base))
        if stage:
            send_sums(stage - 1)
    states_load.wait()
    send_sums(len(stages) - 1)

    def summed(stage):
        lo, n = ranges[stage]
        total = own_sum[:, lo : lo + n]
        for d in range(1, kv):
            second[stage][d - 1].wait_recv()
            total = total + sum_in[d, :, lo : lo + n].astype(f32)
        return total.astype(bf16).astype(f32)[:props]

    part_x = jnp.concatenate([summed(s) for s in range(len(big))], axis=1)
    part_bc = summed(len(big))
    fresh = []
    for g in range(groups):
        fresh.append(
            jnp.concatenate(
                [
                    part_x[:, g * inner : (g + 1) * inner],
                    part_bc[:, g * state : (g + 1) * state],
                    part_bc[:, bc + g * state : bc + (g + 1) * state],
                ],
                axis=1,
            )
        )
        span[g, taps_n - 1 : taps_n - 1 + props] = fresh[g]
    for j in range(props):
        tail_out[0, taps_n - 1 + j] = jnp.concatenate(
            [fresh[g][j : j + 1] for g in range(groups)], axis=0
        ).astype(bf16)

    lhs_rows = [None] * groups
    rhs = [None] * groups
    responses = []
    for g in range(groups):
        conv = jnp.zeros((props, channels), f32)
        for k in range(taps_n):
            conv = conv + span[g, k : k + props] * taps[k].astype(f32)[g : g + 1]
        act = conv * jax.nn.sigmoid(conv)
        x = act[:, :inner]
        b = act[:, inner : inner + state]
        c = act[:, inner + state :]
        cols = slice(g * inner, (g + 1) * inner)
        previous = states[start - 1, g * per_group : (g + 1) * per_group].reshape(inner, state)
        carried = lax.dot_general(
            jnp.concatenate([c, jnp.zeros((16 - props, state), f32)], axis=0).astype(bf16),
            previous.astype(bf16),
            (((1,), (1,)), ((), ())),
            preferred_element_type=f32,
        )
        out_rows = []
        for j in range(props):
            total = expanded[j : j + 1, cols] * carried[j : j + 1]
            total = total + expanded[count - 1 : count, cols] * x[j : j + 1]
            for i in range(j + 1):
                weight = jnp.sum(b[i : i + 1] * c[j : j + 1], axis=-1, keepdims=True)
                at = props + pairs.index((j, i))
                total = total + expanded[at : at + 1, cols] * weight * x[i : i + 1]
            out_rows.append(total)
        responses.append(jnp.concatenate(out_rows, axis=0))
        left, right = [], []
        for j in range(props):
            at = props + pairs.index((j, j))
            scaled = expanded[at : at + 1, cols] * x[j : j + 1]
            xh, xm, _ = split_rows(scaled)
            bh, bm, _ = split_rows(b[j : j + 1])
            left += [xh, xh, xm]
            before = jnp.zeros((1, 128 * j), f32)
            after = jnp.zeros((1, 128 * (props - j) - state), f32)
            for row in (bh, bm, bh):
                right.append(jnp.concatenate(([before] if j else []) + [row, after], axis=1))
        extra = -len(left) % 16
        lhs_rows[g] = jnp.concatenate(left + [jnp.zeros((extra, inner), f32)], axis=0)
        rhs[g] = jnp.concatenate(right + [jnp.zeros((extra, 128 * props), f32)], axis=0)

    gate = jnp.concatenate([summed(len(big) + 1 + s) for s in range(len(big))], axis=1)
    for g in range(groups):
        cols = slice(g * inner, (g + 1) * inner)
        raw = gate[:, cols]
        value = responses[g] * (raw * jax.nn.sigmoid(raw))
        value = value * rms_scale(value) * norm_scale[:, cols]
        value = jnp.concatenate([value, jnp.zeros((rows - props, inner), f32)], axis=0)
        gated_buf[:, cols] = value.astype(bf16)

    third = [
        send(gated_buf, gated_in.at[d], c_send.at[d], c_recv.at[d], {"kv": kv_peer(d)})
        for d in range(1, kv)
    ]

    for g in range(groups):
        outer_buf[g * inner : (g + 1) * inner] = jnp.dot(
            jnp.transpose(lhs_rows[g]).astype(bf16), rhs[g].astype(bf16), preferred_element_type=f32
        )

    def head_step(h, _):
        value = states[start - 1, h]
        for j in range(props):
            outer = outer_buf[pl.ds(pl.multiple_of(h * head_dim, head_dim), head_dim), 128 * j : 128 * j + state]
            value = value * decay_buf[j, pl.ds(h, 1)] + outer
            states_out[0, j, h] = value
        return 0

    lax.fori_loop(0, heads, head_step, 0, unroll=4)

    out_load.wait()
    blocks = [gated_buf[...].astype(f32)]
    for d in range(1, kv):
        third[d - 1].wait_recv()
        blocks.append(gated_in[d].astype(f32))
    everyone = jnp.concatenate(blocks, axis=0).astype(bf16)
    fourth = []
    pieces = lane_chunks(out_w.shape[1], out_w.shape[1] // 2)

    def send_out(piece):
        lo, n = pieces[piece]
        for d in range(1, tp):
            target = lax.rem(me_tp + d, tp)
            fourth.append(
                send(
                    out_buf.at[lax.rem(me + kv - target, kv), :, lo : lo + n],
                    out_in.at[d, :, lo : lo + n],
                    d_send.at[piece, d],
                    d_recv.at[piece, d],
                    {"tp": target},
                )
            )

    for piece, (lo, n) in enumerate(pieces):
        product = jnp.dot(everyone, out_w[:, lo : lo + n], preferred_element_type=f32)
        for d in range(kv):
            out_buf[d, :, lo : lo + n] = product[d * rows : (d + 1) * rows].astype(bf16)
        send_out(piece)
    for copy in fourth:
        copy.wait_recv()
    total = out_buf[lax.rem(me + kv - me_tp, kv)].astype(f32)
    for d in range(1, tp):
        total = total + out_in[d].astype(f32)
    mixed_out[0] = total[:props].astype(bf16)
    for copy in copies:
        copy.wait_send()


def fused(kv, tp, args):
    (
        tokens,
        input_norm_scale,
        head_input_matrix,
        output_gate_matrix,
        group_input_matrix,
        group_readout_matrix,
        step_size_matrix,
        step_size_bias,
        log_decay_rate,
        direct_path_weight,
        convolution_tap_weight,
        convolution_history_rows,
        per_proposal_states,
        accepted,
        proposal_extra_decay,
        group_norm_scale,
        output_projection_matrix,
    ) = args
    _, props, width = tokens.shape
    rows = -(-props // 4) * 4
    heads = step_size_bias.shape[0]
    groups, channels = convolution_tap_weight.shape[1:]
    state = per_proposal_states.shape[4]
    inputs = head_input_matrix.shape[1]
    total = 2 * inputs + 2 * group_input_matrix.shape[1]
    columns = output_projection_matrix.shape[1]
    bf16, f32 = jnp.bfloat16, jnp.float32
    stages = 5
    vmem = pl.BlockSpec(memory_space=pltpu.VMEM)
    hbm = pl.BlockSpec(memory_space=pltpu.HBM)
    dma = pltpu.SemaphoreType.DMA
    return pl.pallas_call(
        functools.partial(mixer_kernel, (kv, tp, rows, props)),
        name="mixer",
        out_shape=(
            pltpu.VMEM((1, props, columns), bf16),
            pltpu.VMEM(per_proposal_states.shape, f32),
            pltpu.VMEM(convolution_history_rows.shape, bf16),
        ),
        in_specs=[pl.BlockSpec(memory_space=pltpu.SMEM)] + [hbm] * 16,
        out_specs=(vmem, vmem, vmem),
        scratch_shapes=[
            pltpu.VMEM(tokens.shape, bf16),
            pltpu.VMEM((1, width), f32),
            pltpu.VMEM((1, heads), f32),
            pltpu.VMEM((1, heads), f32),
            pltpu.VMEM((1, heads), f32),
            pltpu.VMEM(convolution_tap_weight.shape, bf16),
            pltpu.VMEM(convolution_history_rows.shape, bf16),
            pltpu.VMEM((props, 1, heads), f32),
            pltpu.VMEM((1, inputs), f32),
            pltpu.VMEM(head_input_matrix.shape, bf16),
            pltpu.VMEM(output_gate_matrix.shape, bf16),
            pltpu.VMEM(group_input_matrix.shape, bf16),
            pltpu.VMEM(group_readout_matrix.shape, bf16),
            pltpu.VMEM(step_size_matrix.shape[::-1], bf16),
            pltpu.VMEM(per_proposal_states.shape[1:], f32),
            pltpu.VMEM(output_projection_matrix.shape, bf16),
            pltpu.VMEM((kv, rows, width // kv), bf16),
            pltpu.VMEM((kv, rows, width // kv), bf16),
            pltpu.VMEM((rows, total), f32),
            pltpu.VMEM((kv, rows, total), bf16),
            pltpu.VMEM((kv, rows, total), bf16),
            pltpu.VMEM((rows, inputs), bf16),
            pltpu.VMEM((kv, rows, inputs), bf16),
            pltpu.VMEM((kv, rows, columns), bf16),
            pltpu.VMEM((tp, rows, columns), bf16),
            pltpu.VMEM((groups, 8, channels), f32),
            pltpu.VMEM((inputs, 128 * props), f32),
            pltpu.VMEM((props, heads, state), f32),
            dma((19,)),
            dma((kv,)),
            dma((kv,)),
            dma((stages, kv)),
            dma((stages, kv)),
            dma((kv,)),
            dma((kv,)),
            dma((2, tp)),
            dma((2, tp)),
        ],
        compiler_params=pltpu.CompilerParams(
            collective_id=0, has_side_effects=True, vmem_limit_bytes=48 * 1024 * 1024
        ),
    )(
        accepted,
        *[
            pltpu.with_memory_space_constraint(value, pltpu.HBM)
            for value in (
                tokens,
                input_norm_scale[None],
                head_input_matrix,
                output_gate_matrix,
                group_input_matrix,
                group_readout_matrix,
                step_size_matrix.T,
                step_size_bias[None],
                log_decay_rate[None],
                direct_path_weight[None],
                convolution_tap_weight,
                convolution_history_rows,
                per_proposal_states,
                jnp.transpose(proposal_extra_decay, (1, 0, 2)),
                group_norm_scale[None],
                output_projection_matrix,
            )
        ]
    )


def fits(kv, tp, args):
    tokens, taps, states = args[0], args[10], args[12]
    heads = args[7].shape[0]
    slices = (tokens.shape[2] // kv, args[4].shape[1], args[16].shape[1])
    return (
        kv == tp
        and tokens.shape[0] == 1
        and tokens.shape[1] + taps.shape[0] - 1 <= 8
        and heads <= 128
        and states.shape[4] <= 128
        and heads // taps.shape[1] * states.shape[3] % 128 == 0
        and all(n % 256 == 0 or n == slices[1] and n % 128 == 0 for n in slices)
        and args[2].shape[1] % 256 == 0
    )


def solution(mesh):
    kv, tp = mesh.shape["kv"], mesh.shape["tp"]

    def body(*args):
        if fits(kv, tp, args):
            return tuple(fused(kv, tp, args))
        return local(*args)

    return jax.shard_map(
        body,
        mesh=mesh,
        in_specs=(
            P(("grp", "kv"), None, None),
            P(),
            P("kv", "tp"),
            P("kv", "tp"),
            P("kv", "tp"),
            P("kv", "tp"),
            P(None, "tp"),
            P("tp"),
            P("tp"),
            P("tp"),
            P(None, "tp", None),
            P(("grp", "kv"), None, "tp", None),
            P(("grp", "kv"), None, "tp", None, None),
            P(("grp", "kv")),
            P(("grp", "kv"), None, "tp"),
            P("tp"),
            P("tp", "kv"),
        ),
        out_specs=(
            P(("grp", "tp"), None, "kv"),
            P(("grp", "kv"), None, "tp", None, None),
            P(("grp", "kv"), None, "tp", None),
        ),
        check_vma=False,
    )
```

```python
import functools

import jax
import jax.numpy as jnp
from jax import lax
from jax.experimental import pallas as pl
from jax.experimental.pallas import tpu as pltpu
from jax.sharding import PartitionSpec as P

epsilon = 1e-06


def rms_scale(values):
    return lax.rsqrt(jnp.mean(values * values, axis=-1, keepdims=True) + epsilon)


def causal_states(log_decay_factor, head_step_size, ssm_inputs, inject, start_state):
    cumulative = jnp.cumsum(log_decay_factor, axis=1)
    length = log_decay_factor.shape[1]
    lower = (jnp.arange(length)[:, None] >= jnp.arange(length)[None, :])[None, :, :, None]
    spread = cumulative[:, :, None, :] - cumulative[:, None, :, :]
    factors = jnp.where(lower, jnp.exp(jnp.where(lower, spread, 0.0)), 0.0)
    mixing = factors * head_step_size[:, None, :, :]
    carried = jnp.exp(cumulative)[..., None, None] * start_state[:, None]
    return carried + jnp.einsum("sjih,sihp,sihn->sjhpn", mixing, ssm_inputs, inject)


def combine_head_outputs(
    incoming_token_rows,
    gate_portion,
    unactivated_step,
    step_size_bias,
    log_decay_rate,
    direct_path_weight,
    convolution_tap_weight,
    convolution_history_rows,
    per_proposal_states,
    accepted,
    proposal_extra_decay,
    group_norm_scale,
):
    sequences, proposals, group_count, group_width = incoming_token_rows.shape
    head_count = step_size_bias.shape[0]
    head_dim = per_proposal_states.shape[3]
    state_size = per_proposal_states.shape[4]
    per_group = head_count // group_count
    group_inner = per_group * head_dim
    tap_count = convolution_tap_weight.shape[0]
    offsets = accepted[:, None] + jnp.arange(tap_count - 1, dtype=jnp.int32)[None, :]
    context = jnp.take_along_axis(convolution_history_rows, offsets[:, :, None, None], axis=1)
    convolution_span = jnp.concatenate([context, incoming_token_rows], axis=1)
    widened = convolution_span.astype(jnp.float32)
    convolved = jnp.zeros((sequences, proposals, group_count, group_width), jnp.float32)
    for conv_tap in range(tap_count):
        convolved = convolved + widened[
            :, conv_tap : conv_tap + proposals
        ] * convolution_tap_weight[conv_tap].astype(jnp.float32)
    activated = jax.nn.silu(convolved)
    ssm_inputs = activated[..., :group_inner].reshape(sequences, proposals, head_count, head_dim)
    inject = jnp.repeat(activated[..., group_inner : group_inner + state_size], per_group, axis=2)
    readout = jnp.repeat(activated[..., group_inner + state_size :], per_group, axis=2)
    head_step_size = jax.nn.softplus(unactivated_step + step_size_bias)
    log_decay_factor = proposal_extra_decay - jnp.exp(log_decay_rate) * head_step_size
    chosen = (accepted - 1)[:, None, None, None, None]
    start_state = jnp.take_along_axis(per_proposal_states, chosen, axis=1)[:, 0]
    running_state_rows = causal_states(
        log_decay_factor, head_step_size, ssm_inputs, inject, start_state
    )
    response = (
        jnp.einsum("sjhn,sjhpn->sjhp", readout, running_state_rows)
        + direct_path_weight[:, None] * ssm_inputs
    )
    gate_raw = gate_portion.astype(jnp.float32).reshape(sequences, proposals, head_count, head_dim)
    gate_applied_output = (response * jax.nn.silu(gate_raw)).reshape(
        sequences, proposals, group_count, group_inner
    )
    scaled = (
        gate_applied_output
        * rms_scale(gate_applied_output)
        * group_norm_scale.reshape(group_count, group_inner)
    )
    flat_gated = scaled.astype(jnp.bfloat16).reshape(sequences, proposals, head_count * head_dim)
    return (flat_gated, running_state_rows, convolution_span)


def local(
    tokens,
    input_norm_scale,
    head_input_matrix,
    output_gate_matrix,
    group_input_matrix,
    group_readout_matrix,
    step_size_matrix,
    step_size_bias,
    log_decay_rate,
    direct_path_weight,
    convolution_tap_weight,
    convolution_history_rows,
    per_proposal_states,
    accepted,
    proposal_extra_decay,
    group_norm_scale,
    output_projection_matrix,
):
    local_seqs, proposals, width = tokens.shape
    head_local = step_size_bias.shape[0]
    group_local = convolution_tap_weight.shape[1]
    head_dim = per_proposal_states.shape[3]
    state_size = per_proposal_states.shape[4]
    group_inner = head_local // group_local * head_dim
    widened = tokens.astype(jnp.float32)
    normed = (widened * rms_scale(widened) * input_norm_scale).astype(jnp.bfloat16)
    unactivated_step = jnp.einsum(
        "sjd,dh->sjh", normed, step_size_matrix, preferred_element_type=jnp.float32
    )
    pieces = lax.all_to_all(normed, "kv", split_axis=2, concat_axis=0, tiled=True)
    joined = jnp.concatenate(
        [head_input_matrix, group_input_matrix, group_readout_matrix, output_gate_matrix], axis=1
    )
    summed = lax.psum_scatter(
        jnp.einsum("sjd,dc->sjc", pieces, joined, preferred_element_type=jnp.float32),
        "kv",
        scatter_dimension=0,
        tiled=True,
    )
    projected = summed.astype(jnp.bfloat16)
    input_width = head_local * head_dim
    inject_width = group_local * state_size
    part_input = projected[..., :input_width].reshape(
        local_seqs, proposals, group_local, group_inner
    )
    part_inject = projected[..., input_width : input_width + inject_width].reshape(
        local_seqs, proposals, group_local, state_size
    )
    part_readout = projected[
        ..., input_width + inject_width : input_width + 2 * inject_width
    ].reshape(local_seqs, proposals, group_local, state_size)
    gate_portion = projected[..., input_width + 2 * inject_width :]
    incoming_token_rows = jnp.concatenate([part_input, part_inject, part_readout], axis=-1)
    gate_applied_output, running_state_rows, convolution_span = combine_head_outputs(
        incoming_token_rows,
        gate_portion,
        unactivated_step,
        step_size_bias,
        log_decay_rate,
        direct_path_weight,
        convolution_tap_weight,
        convolution_history_rows,
        per_proposal_states,
        accepted,
        proposal_extra_decay,
        group_norm_scale,
    )
    terms = jnp.einsum(
        "sjc,cd->sjd",
        lax.all_gather(gate_applied_output, "kv", axis=0, tiled=True),
        output_projection_matrix,
        preferred_element_type=jnp.float32,
    )
    mixed = lax.psum_scatter(terms.astype(jnp.bfloat16), "tp", scatter_dimension=0, tiled=True)
    return (mixed, running_state_rows, convolution_span)


MESH_ID = pl.DeviceIdType.MESH


def lane_chunks(width, piece):
    return [(lo, min(piece, width - lo)) for lo in range(0, width, piece)]


def split_rows(value):
    high = value.astype(jnp.bfloat16).astype(jnp.float32)
    rest = value - high
    middle = rest.astype(jnp.bfloat16).astype(jnp.float32)
    return high, middle, rest - middle


def mixer_kernel(
    sizes,
    accepted,
    tokens_hbm,
    input_scale_hbm,
    head_hbm,
    gate_hbm,
    inject_hbm,
    readout_hbm,
    step_hbm,
    step_bias_hbm,
    decay_rate_hbm,
    direct_weight_hbm,
    taps_hbm,
    history_hbm,
    states_hbm,
    extra_decay_hbm,
    norm_scale_hbm,
    out_hbm,
    mixed_out,
    states_out,
    tail_out,
    tokens,
    input_scale,
    step_bias,
    decay_rate,
    direct_weight,
    taps,
    history,
    extra_decay,
    norm_scale,
    head_w,
    gate_w,
    inject_w,
    readout_w,
    step_w,
    states,
    out_w,
    normed_buf,
    normed_in,
    own_sum,
    sum_buf,
    sum_in,
    gated_buf,
    gated_in,
    out_buf,
    out_in,
    span,
    outer_buf,
    decay_buf,
    load_sem,
    a_send,
    a_recv,
    b_send,
    b_recv,
    c_send,
    c_recv,
    d_send,
    d_recv,
):
    kv, tp, rows, props = sizes
    width = tokens.shape[-1]
    part = width // kv
    heads = step_bias.shape[-1]
    groups, channels = taps.shape[1:]
    head_dim, state = states.shape[2:]
    per_group = heads // groups
    inner = per_group * head_dim
    inputs = heads * head_dim
    bc = groups * state
    taps_n = taps.shape[0]
    f32 = jnp.float32
    bf16 = jnp.bfloat16
    me = lax.axis_index("kv")
    me_tp = lax.axis_index("tp")

    def kv_peer(d):
        return lax.rem(me + d, kv)

    def kv_source(d):
        return lax.rem(me + kv - d, kv)

    barrier = pltpu.get_barrier_semaphore()
    for d in range(1, kv):
        pl.semaphore_signal(barrier, 1, device_id={"kv": kv_peer(d)}, device_id_type=MESH_ID)
    for d in range(1, tp):
        pl.semaphore_signal(
            barrier, 1, device_id={"tp": lax.rem(me_tp + d, tp)}, device_id_type=MESH_ID
        )

    loads = []

    def load(src, dst):
        copy = pltpu.make_async_copy(src, dst, load_sem.at[len(loads)])
        copy.start()
        loads.append(copy)
        return copy

    token_loads = [load(tokens_hbm, tokens), load(input_scale_hbm, input_scale)]
    step_loads = [
        load(step_hbm, step_w),
        load(step_bias_hbm, step_bias),
        load(decay_rate_hbm, decay_rate),
        load(direct_weight_hbm, direct_weight),
        load(extra_decay_hbm, extra_decay),
    ]
    row_loads = [
        load(history_hbm, history),
        load(taps_hbm, taps),
        load(norm_scale_hbm, norm_scale),
    ]
    big = lane_chunks(inputs, inner)
    group_loads = [load(inject_hbm, inject_w), load(readout_hbm, readout_w)]
    head_loads = [load(head_hbm.at[:, lo : lo + n], head_w.at[:, lo : lo + n]) for lo, n in big]
    gate_loads = [load(gate_hbm.at[:, lo : lo + n], gate_w.at[:, lo : lo + n]) for lo, n in big]
    states_load = load(states_hbm.at[0], states)
    out_load = load(out_hbm, out_w)

    for copy in token_loads:
        copy.wait()
    wide = tokens[0].astype(f32)
    normed = wide * rms_scale(wide) * input_scale[...]
    normed = jnp.concatenate([normed, jnp.zeros((rows - props, width), f32)], axis=0)
    for k in range(kv):
        normed_buf[k] = normed[:, k * part : (k + 1) * part].astype(bf16)
    pl.semaphore_wait(barrier, kv + tp - 2)

    copies = []

    def send(src, dst, send_sem, recv_sem, device):
        copy = pltpu.make_async_remote_copy(
            src_ref=src,
            dst_ref=dst,
            send_sem=send_sem,
            recv_sem=recv_sem,
            device_id=device,
            device_id_type=MESH_ID,
        )
        copy.start()
        copies.append(copy)
        return copy

    first = [
        send(normed_buf.at[kv_peer(d)], normed_in.at[d], a_send.at[d], a_recv.at[d], {"kv": kv_peer(d)})
        for d in range(1, kv)
    ]

    for copy in step_loads:
        copy.wait()
    step_raw = lax.dot_general(
        normed.astype(bf16), step_w[...], (((1,), (1,)), ((), ())), preferred_element_type=f32
    )[:props]
    biased = step_raw + step_bias[...]
    step_size = jnp.maximum(biased, 0.0) + jnp.log1p(jnp.exp(-jnp.abs(biased)))
    rate = jnp.exp(decay_rate[...])
    log_rows = [extra_decay[j] - rate * step_size[j : j + 1] for j in range(props)]
    cumulative = [log_rows[0]]
    for j in range(1, props):
        cumulative.append(cumulative[-1] + log_rows[j])
    pairs = [(j, i) for j in range(props) for i in range(j + 1)]
    stacked = [jnp.exp(row) for row in cumulative]
    stacked += [jnp.exp(cumulative[j] - cumulative[i]) * step_size[i : i + 1] for j, i in pairs]
    stacked.append(direct_weight[...])
    count = len(stacked)
    table = jnp.concatenate(stacked, axis=0)
    padded = -(-3 * count // 16) * 16
    pieces = list(split_rows(table)) + [jnp.zeros((padded - 3 * count, heads), f32)]
    spread = (
        lax.broadcasted_iota(jnp.int32, (heads, inputs), 1) // head_dim
        == lax.broadcasted_iota(jnp.int32, (heads, inputs), 0)
    )
    wide_table = jnp.dot(
        jnp.concatenate(pieces, axis=0).astype(bf16),
        jnp.where(spread, 1.0, 0.0).astype(bf16),
        preferred_element_type=f32,
    )
    expanded = wide_table[:count] + wide_table[count : 2 * count] + wide_table[2 * count : 3 * count]

    dec = jnp.concatenate([jnp.exp(row) for row in log_rows], axis=0)
    dec = jnp.concatenate([dec, jnp.zeros((8 - props, heads), f32)], axis=0)
    dec = jnp.concatenate([dec, jnp.zeros((8, 128 - heads), f32)], axis=1)
    dec_t = jnp.transpose(dec)
    for j in range(props):
        decay_buf[j] = jnp.broadcast_to(dec_t[:heads, j : j + 1], (heads, state))

    for copy in row_loads:
        copy.wait()
    start = jnp.maximum(accepted[0], 1)
    for r in range(taps_n - 1):
        row = history[0, start + r]
        tail_out[0, r] = row
        row = row.astype(f32)
        for g in range(groups):
            span[g, r : r + 1] = row[g : g + 1]

    blocks = [normed_buf[me].astype(f32)]
    for d in range(1, kv):
        first[d - 1].wait_recv()
        blocks.append(normed_in[d].astype(f32))
    gathered = jnp.concatenate(blocks, axis=0).astype(bf16)

    stages = [(inputs, [(inject_w, 0, bc), (readout_w, 0, bc)], group_loads)]
    for at, (lo, n) in enumerate(big):
        stages.append((lo, [(head_w, lo, n)], [head_loads[at]]))
    for at, (lo, n) in enumerate(big):
        stages.append((inputs + 2 * bc + lo, [(gate_w, lo, n)], [gate_loads[at]]))
    second = [[] for _ in stages]
    ranges = []

    def send_sums(stage):
        lo, n = ranges[stage]
        for d in range(1, kv):
            second[stage].append(
                send(
                    sum_buf.at[d, :, lo : lo + n],
                    sum_in.at[d, :, lo : lo + n],
                    b_send.at[stage, d],
                    b_recv.at[stage, d],
                    {"kv": kv_source(d)},
                )
            )

    for stage, (base, operands, ready) in enumerate(stages):
        for copy in ready:
            copy.wait()
        at = base
        for ref, lo, n in operands:
            for sub, size in lane_chunks(n, 512):
                part_sum = jnp.dot(
                    gathered, ref[:, lo + sub : lo + sub + size], preferred_element_type=f32
                )
                own_sum[:, at : at + size] = part_sum[:rows]
                for d in range(1, kv):
                    sum_buf[d, :, at : at + size] = part_sum[d * rows : (d + 1) * rows].astype(bf16)
                at += size
        ranges.append((base, at - base))
        if stage:
            send_sums(stage - 1)
    states_load.wait()
    send_sums(len(stages) - 1)

    def summed(stage):
        lo, n = ranges[stage]
        total = own_sum[:, lo : lo + n]
        for d in range(1, kv):
            second[stage][d - 1].wait_recv()
            total = total + sum_in[d, :, lo : lo + n].astype(f32)
        return total.astype(bf16).astype(f32)[:props]

    part_bc = summed(0)
    fresh, xs, bs, responses = [], [], [], []
    for g in range(groups):
        fresh.append(
            jnp.concatenate(
                [
                    summed(1 + g),
                    part_bc[:, g * state : (g + 1) * state],
                    part_bc[:, bc + g * state : bc + (g + 1) * state],
                ],
                axis=1,
            )
        )
        span[g, taps_n - 1 : taps_n - 1 + props] = fresh[g]
        conv = jnp.zeros((props, channels), f32)
        for k in range(taps_n):
            conv = conv + span[g, k : k + props] * taps[k].astype(f32)[g : g + 1]
        act = conv * jax.nn.sigmoid(conv)
        x = act[:, :inner]
        b = act[:, inner : inner + state]
        c = act[:, inner + state :]
        xs.append(x)
        bs.append(b)
        cols = slice(g * inner, (g + 1) * inner)
        previous = states[start - 1, g * per_group : (g + 1) * per_group].reshape(inner, state)
        carried = lax.dot_general(
            jnp.concatenate([c, jnp.zeros((16 - props, state), f32)], axis=0).astype(bf16),
            previous.astype(bf16),
            (((1,), (1,)), ((), ())),
            preferred_element_type=f32,
        )
        out_rows = []
        for j in range(props):
            total = expanded[j : j + 1, cols] * carried[j : j + 1]
            total = total + expanded[count - 1 : count, cols] * x[j : j + 1]
            for i in range(j + 1):
                weight = jnp.sum(b[i : i + 1] * c[j : j + 1], axis=-1, keepdims=True)
                at = props + pairs.index((j, i))
                total = total + expanded[at : at + 1, cols] * weight * x[i : i + 1]
            out_rows.append(total)
        responses.append(jnp.concatenate(out_rows, axis=0))

    third = []
    for g in range(groups):
        cols = slice(g * inner, (g + 1) * inner)
        raw = summed(1 + groups + g)
        value = responses[g] * (raw * jax.nn.sigmoid(raw))
        value = value * rms_scale(value) * norm_scale[:, cols]
        value = jnp.concatenate([value, jnp.zeros((rows - props, inner), f32)], axis=0)
        gated_buf[:, cols] = value.astype(bf16)
        third.append(
            [
                send(
                    gated_buf.at[:, cols],
                    gated_in.at[d, :, cols],
                    c_send.at[g, d],
                    c_recv.at[g, d],
                    {"kv": kv_peer(d)},
                )
                for d in range(1, kv)
            ]
        )

    for j in range(props):
        tail_out[0, taps_n - 1 + j] = jnp.concatenate(
            [fresh[g][j : j + 1] for g in range(groups)], axis=0
        ).astype(bf16)
    for g in range(groups):
        cols = slice(g * inner, (g + 1) * inner)
        left, right = [], []
        for j in range(props):
            at = props + pairs.index((j, j))
            xh, xm, _ = split_rows(expanded[at : at + 1, cols] * xs[g][j : j + 1])
            bh, bm, _ = split_rows(bs[g][j : j + 1])
            left += [xh, xh, xm]
            before = jnp.zeros((1, 128 * j), f32)
            after = jnp.zeros((1, 128 * (props - j) - state), f32)
            for row in (bh, bm, bh):
                right.append(jnp.concatenate(([before] if j else []) + [row, after], axis=1))
        extra = -len(left) % 16
        left = jnp.concatenate(left + [jnp.zeros((extra, inner), f32)], axis=0)
        right = jnp.concatenate(right + [jnp.zeros((extra, 128 * props), f32)], axis=0)
        outer_buf[cols] = jnp.dot(
            jnp.transpose(left).astype(bf16), right.astype(bf16), preferred_element_type=f32
        )

    def head_step(h, _):
        value = states[start - 1, h]
        for j in range(props):
            outer = outer_buf[pl.ds(pl.multiple_of(h * head_dim, head_dim), head_dim), 128 * j : 128 * j + state]
            value = value * decay_buf[j, pl.ds(h, 1)] + outer
            states_out[0, j, h] = value
        return 0

    lax.fori_loop(0, heads, head_step, 0, unroll=4)

    out_load.wait()
    everyone = []
    for g in range(groups):
        cols = slice(g * inner, (g + 1) * inner)
        blocks = [gated_buf[:, cols].astype(f32)]
        for d in range(1, kv):
            third[g][d - 1].wait_recv()
            blocks.append(gated_in[d, :, cols].astype(f32))
        everyone.append(jnp.concatenate(blocks, axis=0).astype(bf16))
    everyone = jnp.concatenate(everyone, axis=1)
    fourth = []
    pieces = lane_chunks(out_w.shape[1], out_w.shape[1] // 2)

    def send_out(piece):
        lo, n = pieces[piece]
        for d in range(1, tp):
            target = lax.rem(me_tp + d, tp)
            fourth.append(
                send(
                    out_buf.at[lax.rem(me + kv - target, kv), :, lo : lo + n],
                    out_in.at[d, :, lo : lo + n],
                    d_send.at[piece, d],
                    d_recv.at[piece, d],
                    {"tp": target},
                )
            )

    for piece, (lo, n) in enumerate(pieces):
        product = jnp.dot(everyone, out_w[:, lo : lo + n], preferred_element_type=f32)
        for d in range(kv):
            out_buf[d, :, lo : lo + n] = product[d * rows : (d + 1) * rows].astype(bf16)
        send_out(piece)
    for copy in fourth:
        copy.wait_recv()
    total = out_buf[lax.rem(me + kv - me_tp, kv)].astype(f32)
    for d in range(1, tp):
        total = total + out_in[d].astype(f32)
    mixed_out[0] = total[:props].astype(bf16)
    for copy in copies:
        copy.wait_send()


def fused(kv, tp, args):
    (
        tokens,
        input_norm_scale,
        head_input_matrix,
        output_gate_matrix,
        group_input_matrix,
        group_readout_matrix,
        step_size_matrix,
        step_size_bias,
        log_decay_rate,
        direct_path_weight,
        convolution_tap_weight,
        convolution_history_rows,
        per_proposal_states,
        accepted,
        proposal_extra_decay,
        group_norm_scale,
        output_projection_matrix,
    ) = args
    _, props, width = tokens.shape
    rows = -(-props // 4) * 4
    heads = step_size_bias.shape[0]
    groups, channels = convolution_tap_weight.shape[1:]
    state = per_proposal_states.shape[4]
    inputs = head_input_matrix.shape[1]
    total = 2 * inputs + 2 * group_input_matrix.shape[1]
    columns = output_projection_matrix.shape[1]
    bf16, f32 = jnp.bfloat16, jnp.float32
    stages = 1 + 2 * groups
    vmem = pl.BlockSpec(memory_space=pltpu.VMEM)
    hbm = pl.BlockSpec(memory_space=pltpu.HBM)
    dma = pltpu.SemaphoreType.DMA
    results = pl.pallas_call(
        functools.partial(mixer_kernel, (kv, tp, rows, props)),
        name="mixer",
        out_shape=(
            pltpu.VMEM((1, props, columns), bf16),
            pltpu.VMEM(per_proposal_states.shape, f32),
            pltpu.VMEM(convolution_history_rows.shape, bf16),
        ),
        in_specs=[pl.BlockSpec(memory_space=pltpu.SMEM)] + [hbm] * 16,
        out_specs=(vmem, vmem, vmem),
        scratch_shapes=[
            pltpu.VMEM(tokens.shape, bf16),
            pltpu.VMEM((1, width), f32),
            pltpu.VMEM((1, heads), f32),
            pltpu.VMEM((1, heads), f32),
            pltpu.VMEM((1, heads), f32),
            pltpu.VMEM(convolution_tap_weight.shape, bf16),
            pltpu.VMEM(convolution_history_rows.shape, bf16),
            pltpu.VMEM((props, 1, heads), f32),
            pltpu.VMEM((1, inputs), f32),
            pltpu.VMEM(head_input_matrix.shape, bf16),
            pltpu.VMEM(output_gate_matrix.shape, bf16),
            pltpu.VMEM(group_input_matrix.shape, bf16),
            pltpu.VMEM(group_readout_matrix.shape, bf16),
            pltpu.VMEM(step_size_matrix.shape[::-1], bf16),
            pltpu.VMEM(per_proposal_states.shape[1:], f32),
            pltpu.VMEM(output_projection_matrix.shape, bf16),
            pltpu.VMEM((kv, rows, width // kv), bf16),
            pltpu.VMEM((kv, rows, width // kv), bf16),
            pltpu.VMEM((rows, total), f32),
            pltpu.VMEM((kv, rows, total), bf16),
            pltpu.VMEM((kv, rows, total), bf16),
            pltpu.VMEM((rows, inputs), bf16),
            pltpu.VMEM((kv, rows, inputs), bf16),
            pltpu.VMEM((kv, rows, columns), bf16),
            pltpu.VMEM((tp, rows, columns), bf16),
            pltpu.VMEM((groups, 8, channels), f32),
            pltpu.VMEM((inputs, 128 * props), f32),
            pltpu.VMEM((props, heads, state), f32),
            dma((14 + 2 * groups,)),
            dma((kv,)),
            dma((kv,)),
            dma((stages, kv)),
            dma((stages, kv)),
            dma((groups, kv)),
            dma((groups, kv)),
            dma((2, tp)),
            dma((2, tp)),
        ],
        compiler_params=pltpu.CompilerParams(
            collective_id=0, has_side_effects=True, vmem_limit_bytes=48 * 1024 * 1024
        ),
    )(
        accepted,
        *[
            pltpu.with_memory_space_constraint(value, pltpu.HBM)
            for value in (
                tokens,
                input_norm_scale[None],
                head_input_matrix,
                output_gate_matrix,
                group_input_matrix,
                group_readout_matrix,
                step_size_matrix.T,
                step_size_bias[None],
                log_decay_rate[None],
                direct_path_weight[None],
                convolution_tap_weight,
                convolution_history_rows,
                per_proposal_states,
                jnp.transpose(proposal_extra_decay, (1, 0, 2)),
                group_norm_scale[None],
                output_projection_matrix,
            )
        ]
    )
    return pl.pallas_call(
        place_kernel,
        name="place",
        out_shape=tuple(jax.ShapeDtypeStruct(r.shape, r.dtype) for r in results),
        in_specs=[vmem] * 3,
        out_specs=(hbm, hbm, hbm),
        scratch_shapes=[dma((2 + props,))],
    )(*[pltpu.with_memory_space_constraint(value, pltpu.VMEM) for value in results])


def place_kernel(*refs):
    sems = refs[-1]
    sources, targets = refs[:3], refs[3:6]
    copies = []
    for source, target in zip(sources, targets):
        parts = range(source.shape[1]) if len(source.shape) == 5 else [None]
        for part in parts:
            view = (lambda ref: ref) if part is None else (lambda ref: ref.at[:, part])
            copy = pltpu.make_async_copy(view(source), view(target), sems.at[len(copies)])
            copy.start()
            copies.append(copy)
    for copy in copies:
        copy.wait()


def fits(kv, tp, args):
    tokens, taps, states = args[0], args[10], args[12]
    heads = args[7].shape[0]
    slices = (tokens.shape[2] // kv, args[4].shape[1], args[16].shape[1])
    return (
        kv == tp
        and tokens.shape[0] == 1
        and tokens.shape[1] + taps.shape[0] - 1 <= 8
        and heads <= 128
        and states.shape[4] <= 128
        and heads // taps.shape[1] * states.shape[3] % 128 == 0
        and all(n % 256 == 0 or n == slices[1] and n % 128 == 0 for n in slices)
        and args[2].shape[1] % 256 == 0
    )


def solution(mesh):
    kv, tp = mesh.shape["kv"], mesh.shape["tp"]

    def body(*args):
        if fits(kv, tp, args):
            return tuple(fused(kv, tp, args))
        return local(*args)

    return jax.shard_map(
        body,
        mesh=mesh,
        in_specs=(
            P(("grp", "kv"), None, None),
            P(),
            P("kv", "tp"),
            P("kv", "tp"),
            P("kv", "tp"),
            P("kv", "tp"),
            P(None, "tp"),
            P("tp"),
            P("tp"),
            P("tp"),
            P(None, "tp", None),
            P(("grp", "kv"), None, "tp", None),
            P(("grp", "kv"), None, "tp", None, None),
            P(("grp", "kv")),
            P(("grp", "kv"), None, "tp"),
            P("tp"),
            P("tp", "kv"),
        ),
        out_specs=(
            P(("grp", "tp"), None, "kv"),
            P(("grp", "kv"), None, "tp", None, None),
            P(("grp", "kv"), None, "tp", None),
        ),
        check_vma=False,
    )
```
